256 devices in a mesh: ep: 16 (over y, x), tp: 16 (over z, core).
Axes of the slice: x: 4, y: 4, z: 8, core: 2. Of those that a mesh axis runs over, the one named last changes fastest.
Arguments:
- queries: bfloat16 [12288, 2048], P('ep', 'tp'), may hold values from -6 to 6
- values: bfloat16 [12288, 2048], P('ep', 'tp'), may hold values from -6 to 6
- forget_gate_logits: bfloat16 [2, 12288, 2048], P(None, 'ep', 'tp'), may hold values from -5 to 5
- output_gate_logits: bfloat16 [12288, 2048], P('ep', 'tp'), may hold values from -6 to 6
- forget_gate_headroom: float32 [2, 2048], P(None, 'tp'), may hold values from 0 to 0.1, as said below
- spike_log_decay: float32 [12288], P('ep'), may hold values from -1.6 to 0
- head_norm_gain: float32 [2048], P('tp'), may hold values from 0.1 to 1.9
- output_projection: bfloat16 [2048, 2048], P(None, 'tp'), may hold values from -0.125 to 0.125
- second_micro_input: bfloat16 [12288, 2048], P('ep'), may hold values from -170 to 170
- expert_norm_gain: float32 [2048], replicated, may hold values from 0.1 to 1.9
- token_group_index: int32 [12288], P('ep'), may hold values from 0 to 7, as said below
- token_expert_pair: int32 [12288, 2], P('ep'), may hold values from 0 to 3, as said below
- group_router_scores: float32 [12288, 8], P('ep'), may hold values from -6 to 320
- expert_router_scores: float32 [12288, 2], P('ep'), may hold values from -6 to 6
- expert_gate_weight: bfloat16 [32, 2048, 4096], P('ep', None, 'tp'), may hold values from -0.125 to 0.125
- expert_up_weight: bfloat16 [32, 2048, 4096], P('ep', None, 'tp'), may hold values from -0.125 to 0.125
- expert_down_weight: bfloat16 [32, 4096, 2048], P('ep', 'tp'), may hold values from -1.25 to 1.25
Outputs:
- recurrence_output: bfloat16 [12288, 2048], P('ep', 'tp')
- expert_tokens: bfloat16 [12288, 2048], P('ep', 'tp')
The draws below stay inside these ranges and needn't reach their ends.
Inputs may be any that keep to these rules, and one draw needn't show every extreme that they name: `token_group_index`: within the rows of one device each of the 8 groups is named by the same number of rows. The two entries of a row differ. Within the rows of one device every expert token_group_index * 4 + token_expert_pair is named exactly 48 times. `forget_gate_headroom`: Positive.
All inputs are finite; a program needn't handle non-finite values.
Results may differ from the reference program's by a relative error of at most 0.018.
Values may be sent and summed in bfloat16 or wider, within the bound.
A program may use at most 128 MiB of HBM per device.

```python
import math
import jax
import jax.numpy as jnp
from jax import lax

D = 2048
HEADS = 16
HEAD_DIM = 128
HG = 2048
FF = 4096
GROUP_EXP = 4
EXPERTS = 32
GROUPS = 8
BLOCK = 64
TOK_EP = 768
MICRO_TOKENS = 12288
N_TP = 16


def draw_forget_gate_logits(key, part):
    base_key, shift_key = jax.random.split(jax.random.fold_in(key, 3))
    block_count = MICRO_TOKENS // TOK_EP
    shifts = jax.random.uniform(shift_key, (2, block_count, 1, 1), jnp.float32, -1.5, 1.5)
    noise_part = jax.random.normal(base_key, (2, block_count, TOK_EP, HG), jnp.float32)
    return jnp.clip(noise_part + shifts, -5.0, 5.0).reshape(2, MICRO_TOKENS, HG).astype(jnp.bfloat16)


def draw_forget_gate_headroom(key, part):
    head_key, slow_key, fast_key, chan_key = jax.random.split(jax.random.fold_in(key, 5), 4)
    fast_head = jax.random.randint(head_key, (2, HEADS, 1), 0, 2) == 1
    slow_gap = jax.random.uniform(slow_key, (2, HEADS, 1), jnp.float32, 0.2, 1.0) / MICRO_TOKENS
    fast_gap = jax.random.uniform(fast_key, (2, HEADS, 1), jnp.float32, 0.04, 0.1)
    spread = jax.random.uniform(chan_key, (2, HEADS, HEAD_DIM), jnp.float32, 0.7, 1.0)
    return (jnp.where(fast_head, fast_gap, slow_gap) * spread).reshape(2, HG).astype(jnp.float32)


def draw_spike_log_decay(key, part):
    position_random_key, strength_random_key = jax.random.split(jax.random.fold_in(key, 9))
    spike_positions = jax.random.randint(position_random_key, (3,), 0, MICRO_TOKENS)
    spike_strength = jax.random.uniform(strength_random_key, (3,), jnp.float32, math.log(0.6), math.log(0.8))
    spike_position_mask = jnp.arange(MICRO_TOKENS)[:, None] == spike_positions[None, :]
    return jnp.sum(jnp.where(spike_position_mask, spike_strength[None, :], 0.0), axis=1).astype(jnp.float32)


def draw_second_micro_input(key, part):
    noise_key, row_key, col_key = jax.random.split(jax.random.fold_in(key, 13), 3)
    row_scale = jnp.exp(jax.random.uniform(row_key, (MICRO_TOKENS, 1), jnp.float32, 0.0, math.log(10.0)))
    col_scale = jnp.exp(jax.random.uniform(col_key, (1, D), jnp.float32, 0.0, math.log(10.0)))
    noise_part = jax.random.normal(noise_key, (MICRO_TOKENS, D), jnp.float32)
    return (jnp.clip(noise_part, -5.0, 5.0) * row_scale * col_scale / 3.0).astype(jnp.bfloat16)


def draw_group_router_scores(key, part):
    base_key = jax.random.fold_in(jax.random.fold_in(key, 17), 0)
    return jnp.clip(1.5 * jax.random.normal(base_key, (MICRO_TOKENS, GROUPS), jnp.float32), -6.0, 6.0)


def block_perm(block_key):
    return jax.random.permutation(block_key, TOK_EP)


def route_table(key):
    perm_key, shift_key = jax.random.split(jax.random.fold_in(key, 23))
    block_count = MICRO_TOKENS // TOK_EP
    places = jax.vmap(block_perm)(jax.random.split(perm_key, block_count)).astype(jnp.int32)
    group_ids = places % GROUPS
    within = places // GROUPS
    shifts = jax.random.randint(shift_key, (block_count, GROUPS), 1, GROUP_EXP)
    step_size = jnp.take_along_axis(shifts, group_ids, axis=1)
    first_inner = within % GROUP_EXP
    second_inner = (within + step_size) % GROUP_EXP
    inner_ids = jnp.stack([first_inner, second_inner], -1).reshape(MICRO_TOKENS, 2)
    return (group_ids.reshape(MICRO_TOKENS).astype(jnp.int32), inner_ids.astype(jnp.int32))


def draw_token_group_index(key, part):
    return route_table(key)[0]


def draw_token_expert_pair(key, part):
    return route_table(key)[1]


def with_spikes(array, rng, source, target, blocks, factor):
    owner, partner = [(jnp.arange(array.shape[axis_at]) // (array.shape[axis_at] // blocks)).reshape([-1 if axis == axis_at else 1 for axis in range(array.ndim)]) for axis_at in (source, target)]
    chosen = jax.random.permutation(rng, blocks)[partner]
    strong = (owner == chosen) | (owner == (partner + blocks // 2) % blocks)
    return jnp.where(strong, factor * array, array)


def shard_levels(stream_key, extent, shards, smallest, high):
    gain, own = 1.0, jax.random.fold_in(stream_key, 6)
    for dim, parts in shards:
        steps = jnp.exp(jax.random.uniform(jax.random.fold_in(own, dim), (parts,), jnp.float32, smallest / len(shards), high / len(shards)))
        gain = gain * jnp.repeat(steps, extent[dim] // parts).reshape([-1 if axis == dim else 1 for axis in range(len(extent))])
    return gain


def scatter_about(rng, dims, deviation, most, shards=(), kind=jnp.bfloat16):
    array = jax.random.normal(rng, dims, jnp.float32) * deviation
    if len(shards) > 0:
        array = shard_levels(rng, dims, shards, -0.22, 0.18) * array
    return jnp.clip(array, min=-most, max=most).astype(kind)


def noise_with(key, extent, scale, most, shards, heavy, held_as=jnp.bfloat16):
    drawn = scale * jax.random.normal(key, extent, jnp.float32)
    if shards:
        drawn = drawn * shard_levels(key, extent, shards, -0.22, 0.18)
    return jnp.clip(with_spikes(drawn, jax.random.fold_in(key, 3), *heavy), -most, most).astype(held_as)


def setup_inputs(seed: int = 0) -> dict:
    arg_keys = jax.random.split(jax.random.key(seed), 18)
    queries = scatter_about(arg_keys[0], (MICRO_TOKENS, HG), 1.0, 6.0, ((0, 16), (1, 16)))
    values = scatter_about(arg_keys[1], (MICRO_TOKENS, HG), 1.0, 6.0, ((0, 16), (1, 16)))
    forget_gate_logits = draw_forget_gate_logits(jax.random.fold_in(arg_keys[17], 71), 0)
    output_gate_logits = scatter_about(arg_keys[3], (MICRO_TOKENS, HG), 1.0, 6.0, ((0, 16), (1, 16)))
    forget_gate_headroom = draw_forget_gate_headroom(jax.random.fold_in(arg_keys[17], 71), 0)
    spike_log_decay = draw_spike_log_decay(jax.random.fold_in(arg_keys[17], 71), 0)
    head_norm_gain = jnp.clip(1.0 + 0.18 * jax.random.normal(arg_keys[6], (HG,), jnp.float32), 0.1, 1.9)
    output_projection = scatter_about(arg_keys[7], (HG, D), HG ** -0.5, 0.125, ((1, 16),))
    second_micro_input = draw_second_micro_input(jax.random.fold_in(arg_keys[17], 71), 0)
    expert_norm_gain = jnp.clip(1.0 + 0.18 * jax.random.normal(arg_keys[9], (D,), jnp.float32), 0.1, 1.9)
    token_group_index = draw_token_group_index(jax.random.fold_in(arg_keys[17], 71), 0)
    token_expert_pair = draw_token_expert_pair(jax.random.fold_in(arg_keys[17], 71), 0)
    group_router_scores = draw_group_router_scores(jax.random.fold_in(arg_keys[17], 71), 0)
    expert_router_scores = scatter_about(arg_keys[13], (MICRO_TOKENS, 2), 1.5, 6.0, ((0, 16),), jnp.float32)
    expert_gate_weight = scatter_about(arg_keys[14], (EXPERTS, D, FF), D ** -0.5, 0.125, ((0, 16), (2, 16)))
    expert_up_weight = scatter_about(arg_keys[15], (EXPERTS, D, FF), D ** -0.5, 0.125, ((0, 16), (2, 16)))
    expert_down_weight = noise_with(arg_keys[16], (EXPERTS, FF, D), (4.0 * FF ** -0.5), 1.25, ((0, 16), (1, 16)), (1, 2, 16, 2.0))
    return dict(queries=queries, values=values, forget_gate_logits=forget_gate_logits, output_gate_logits=output_gate_logits, forget_gate_headroom=forget_gate_headroom, spike_log_decay=spike_log_decay, head_norm_gain=head_norm_gain, output_projection=output_projection, second_micro_input=second_micro_input, expert_norm_gain=expert_norm_gain, token_group_index=token_group_index, token_expert_pair=token_expert_pair, group_router_scores=group_router_scores, expert_router_scores=expert_router_scores, expert_gate_weight=expert_gate_weight, expert_up_weight=expert_up_weight, expert_down_weight=expert_down_weight)


HEAD_EPS = 1e-06
NORM_EPS = 1e-05
FULL_PRECISION = lax.Precision.HIGHEST

def decay_pieces(forget_gate_logits, forget_gate_headroom, spike_log_decay):
    logits = forget_gate_logits.astype(jnp.float32)
    gap_span = forget_gate_headroom[:, None, :]
    logarithm_decay = jnp.logaddexp(jnp.log1p(-gap_span), jnp.log(gap_span) + jax.nn.log_sigmoid(logits))
    logarithm_decay = logarithm_decay + spike_log_decay[None, :, None]
    key_contributions = gap_span * jax.nn.sigmoid(-logits)
    return (logarithm_decay, key_contributions)

def recurrence(lifted, key_contributions, logarithm_decay, inputs_f):
    length = lifted.shape[0]

    def blocked(tensor):
        return tensor.reshape(length // BLOCK, BLOCK, HEADS, HEAD_DIM)
    causal = jnp.tril(jnp.ones((BLOCK, BLOCK), bool))[:, :, None, None]

    def block_step(carried_state, packed):
        block_of_queries, block_of_keys, decay_block, block_of_values = packed
        running_state = jnp.cumsum(decay_block, axis=0)
        spread = running_state[:, None] - running_state[None, :]
        weight = jnp.where(causal, jnp.exp(jnp.where(causal, spread, 0.0)), 0.0)
        scores = lax.optimization_barrier(jnp.sum(block_of_queries[:, None] * block_of_keys[None, :] * weight, axis=-1))
        inner_out = jnp.einsum('tsh,shv->thv', scores, block_of_values, precision=FULL_PRECISION)
        across_block_output = jnp.einsum('gwm,wma->gwa', block_of_queries * jnp.exp(running_state), carried_state, precision=FULL_PRECISION)
        final_block_row = running_state[-1]
        written_output = jnp.einsum('qnx,qnb->nxb', block_of_keys * jnp.exp(final_block_row[None] - running_state), block_of_values, precision=FULL_PRECISION)
        return (jnp.exp(final_block_row)[:, :, None] * carried_state + written_output, inner_out + across_block_output)
    zero_state = jnp.zeros((HEADS, HEAD_DIM, HEAD_DIM), jnp.float32)
    scanned = lax.scan(block_step, zero_state, (blocked(lifted), blocked(key_contributions), blocked(logarithm_decay), blocked(inputs_f)))
    return scanned[1].reshape(length, HEADS, HEAD_DIM)

def recurrence_portion(queries, values, forget_gate_logits, output_gate_logits, forget_gate_headroom, spike_log_decay, head_norm_gain, output_projection):
    length = queries.shape[0]
    logarithm_decay, key_contributions = decay_pieces(forget_gate_logits, forget_gate_headroom, spike_log_decay)

    def heads_of(tensor):
        return tensor.reshape(length, HEADS, HEAD_DIM)
    lifted = heads_of(jax.nn.silu(queries.astype(jnp.float32)))
    inputs_f = heads_of(values.astype(jnp.float32))
    forward_out = recurrence(lifted, heads_of(key_contributions[0]), heads_of(logarithm_decay[0]), inputs_f)
    backward_out = jnp.flip(recurrence(jnp.flip(lifted, 0), jnp.flip(heads_of(key_contributions[1]), 0), jnp.flip(heads_of(logarithm_decay[1]), 0), jnp.flip(inputs_f, 0)), 0)
    joined = forward_out + backward_out
    normed = joined * lax.rsqrt(lax.optimization_barrier(jnp.mean(joined * joined, -1, keepdims=True)) + HEAD_EPS)
    readout = (normed.reshape(length, HG) * head_norm_gain * jax.nn.silu(output_gate_logits.astype(jnp.float32))).astype(jnp.bfloat16)
    return jnp.dot(readout, output_projection, preferred_element_type=jnp.float32).astype(jnp.bfloat16)

def expert_half(second_micro_input, expert_norm_gain, token_group_index, token_expert_pair, group_router_scores, expert_router_scores, expert_gate_weight, expert_up_weight, expert_down_weight):
    count = second_micro_input.shape[0]
    features = second_micro_input.astype(jnp.float32)
    centred = features - lax.optimization_barrier(jnp.mean(features, -1, keepdims=True))
    normed_input = (centred * lax.rsqrt(lax.optimization_barrier(jnp.mean(centred * centred, -1, keepdims=True)) + NORM_EPS) * expert_norm_gain).astype(jnp.bfloat16)
    group_prob = jax.nn.softmax(group_router_scores, axis=-1)
    chosen = lax.optimization_barrier(jnp.sum(jnp.where(jnp.arange(GROUPS)[None, :] == token_group_index[:, None], group_prob, 0.0), -1))
    pair_weight = jnp.stack([jax.nn.sigmoid(expert_router_scores[:, 0] - expert_router_scores[:, 1]), jax.nn.sigmoid(expert_router_scores[:, 1] - expert_router_scores[:, 0])], -1) * chosen[:, None]
    expert_id = (token_group_index[:, None] * GROUP_EXP + token_expert_pair).reshape(-1).astype(jnp.int32)
    order = jnp.argsort(expert_id, stable=True).astype(jnp.int32)
    per_expert = order.reshape(EXPERTS, -1)
    shard_width = FF // N_TP

    def one_expert(packed):
        copy_ids, gate_weight, up_weight, down_weight = packed
        rows_in = normed_input[copy_ids // 2]
        gate_terms = jnp.dot(rows_in, gate_weight, preferred_element_type=jnp.float32)
        up_terms = jnp.dot(rows_in, up_weight, preferred_element_type=jnp.float32)
        hidden = (jax.nn.silu(gate_terms) * up_terms).astype(jnp.bfloat16)
        pieces = jnp.einsum('msf,sfd->smd', hidden.reshape(-1, N_TP, shard_width).astype(jnp.float32), down_weight.reshape(N_TP, shard_width, D).astype(jnp.float32))
        rounded = lax.optimization_barrier(pieces.astype(jnp.bfloat16))
        return lax.optimization_barrier(jnp.sum(rounded.astype(jnp.float32), axis=0)).astype(jnp.bfloat16)
    outputs = lax.map(one_expert, (per_expert, expert_gate_weight, expert_up_weight, expert_down_weight))
    copies = jnp.zeros((2 * count, D), jnp.bfloat16).at[per_expert.reshape(-1)].set(outputs.reshape(-1, D))
    copies = copies.reshape(count, 2, D).astype(jnp.float32)
    return lax.optimization_barrier(jnp.sum(copies * pair_weight[:, :, None], axis=1)).astype(jnp.bfloat16)

def reference(queries, values, forget_gate_logits, output_gate_logits, forget_gate_headroom, spike_log_decay, head_norm_gain, output_projection, second_micro_input, expert_norm_gain, token_group_index, token_expert_pair, group_router_scores, expert_router_scores, expert_gate_weight, expert_up_weight, expert_down_weight):
    recurrence_output = recurrence_portion(queries, values, forget_gate_logits, output_gate_logits, forget_gate_headroom, spike_log_decay, head_norm_gain, output_projection)
    expert_tokens = expert_half(second_micro_input, expert_norm_gain, token_group_index, token_expert_pair, group_router_scores, expert_router_scores, expert_gate_weight, expert_up_weight, expert_down_weight)
    return (recurrence_output, expert_tokens)
```

```python
import functools

import jax
import jax.numpy as jnp
from jax import lax
from jax.experimental import pallas as pl
from jax.experimental.pallas import tpu as pltpu
from jax.sharding import Mesh
from jax.sharding import PartitionSpec as P

HEAD_DIM = 128
GROUP_EXP = 4
BLOCK = 64
TP = ("tp_0", "tp_1")


HEAD_EPS = 1e-06
NORM_EPS = 1e-05


def from_everyone(value, axis):
    copies = jnp.broadcast_to(value, (lax.axis_size(axis), *value.shape))
    return lax.all_to_all(copies, axis, split_axis=0, concat_axis=0, tiled=True)


def collected_together(value, axis):
    leaves = jax.tree.leaves(value)
    order = sorted(range(len(leaves)), key=lambda k: -leaves[k].size)
    width = (1, *leaves[order[0]].shape)[-1]
    lines = [
        jnp.pad(leaves[k].reshape(-1), (0, -leaves[k].size % width)).reshape(-1, width)
        for k in order
    ]
    both, at, found = (from_everyone(jnp.concatenate(lines), axis), 0, {})
    for k, line in zip(order, lines):
        piece = both[:, at : at + len(line)].reshape(len(both), -1)
        found[k] = piece[:, : leaves[k].size].reshape(-1, *leaves[k].shape)
        at += len(line)
    numbers = iter(range(len(leaves)))
    return jax.tree.map(lambda _: found[next(numbers)], value)


def joined_by_halves(pieces, combine):
    while len(jax.tree.leaves(pieces)[0]) > 1:
        pieces = jax.vmap(combine)(
            *(jax.tree.map(lambda part: part[side::2], pieces) for side in (0, 1))
        )
    return jax.tree.map(lambda part: part[0], pieces)


def prefix(value, axis, combine, identity, reverse):
    count, place = (lax.axis_size(axis), lax.axis_index(axis))
    passed = jnp.arange(count) > place if reverse else jnp.arange(count) < place

    def kept(part, zero, own):
        part = jnp.where(
            passed.reshape(-1, *(1 for _ in own.shape)),
            part.astype(own.dtype),
            jnp.asarray(zero, own.dtype),
        )
        return part[::-1] if reverse else part

    pieces = collected_together(
        jax.tree.map(lambda part, kind: part.astype(kind), value, (jnp.bfloat16, jnp.bfloat16)),
        axis,
    )
    return joined_by_halves(jax.tree.map(kept, pieces, identity, value), combine)


def decay_pieces(forget_gate_logits, forget_gate_headroom, spike_log_decay):
    logits = forget_gate_logits.astype(jnp.float32)
    gap_span = forget_gate_headroom[:, None, :]
    logarithm_decay = jnp.logaddexp(
        jnp.log1p(-gap_span), jnp.log(gap_span) + jax.nn.log_sigmoid(logits)
    )
    logarithm_decay = logarithm_decay + spike_log_decay[None, :, None]
    key_contributions = gap_span * jax.nn.sigmoid(-logits)
    return (logarithm_decay, key_contributions)


def combine_states(earlier, following):
    return (earlier[0] + following[0], jnp.exp(following[0])[..., None] * earlier[1] + following[1])


F32, BF16 = jnp.float32, jnp.bfloat16
RINGS = ((0, 0), (0, 1), (1, 0), (1, 1))


def mm(a, b):
    return jnp.dot(a, b, preferred_element_type=F32)


def expert_kernel(
    x_hbm, gain, eid_row, eid_col, weight_col, wg_hbm, wu_hbm, wd_hbm, out,
    x, normed, wg, wu, wd, rank_row, send_buf, arrived, partial, pair_buf,
    ring_buf, final_buf, ret, pick0, pick1,
    load_sem, disp_send, disp_recv, fwd_send, fwd_recv, pair_send, pair_recv,
    ring_send, ring_recv, ret_send, ret_recv,
):
    side = arrived.shape[1]
    cap = arrived.shape[3]
    zs = partial.shape[1]
    rows, width = x.shape
    group_rows = side * cap
    ep_size = side * side
    experts = 2 * ep_size
    me, z, core = lax.axis_index("ep"), lax.axis_index("tp_0"), lax.axis_index("tp_1")
    my_y, my_x = me // side, me % side
    loads = [
        pltpu.make_async_copy(a, b, load_sem.at[n])
        for n, (a, b) in enumerate(((x_hbm, x), (wg_hbm, wg), (wu_hbm, wu), (wd_hbm, wd)))
    ]
    for load in loads:
        load.start()

    barrier = pltpu.get_barrier_semaphore()

    def greet(n, carry):
        pl.semaphore_signal(barrier, 1, device_id={"ep": (me + n) % ep_size})
        return carry

    lax.fori_loop(1, ep_size, greet, 0)
    pl.semaphore_signal(barrier, 1, device_id={"tp_1": 1 - core})
    pl.semaphore_signal(barrier, 1, device_id={"tp_0": (z + 1) % zs})
    pl.semaphore_signal(barrier, 1, device_id={"tp_0": (z + zs - 1) % zs})

    def target(k, m):
        return ((my_y + 2 * side - (m + k) % side) % side) * side + (my_x + side - m) % side

    def source(k, m):
        return ((my_y + (m + k) % side) % side) * side + (my_x + m) % side

    first = lax.broadcasted_iota(jnp.int32, (rows, rows), 0)
    second = lax.broadcasted_iota(jnp.int32, (rows, rows), 1)
    ids = lax.broadcasted_iota(jnp.int32, (experts, rows), 0)
    named = (ids == eid_row[0:1, :]) | (ids == eid_row[1:2, :])
    before = jnp.where(first < second, 1.0, 0.0).astype(BF16)
    rank = mm(jnp.where(named, 1.0, 0.0).astype(BF16), before)
    rank_row[...] = jnp.where(named, rank, -1.0)
    ids_col = lax.broadcasted_iota(jnp.int32, (rows, experts), 1)
    is0, is1 = ids_col == eid_col[:, 0:1], ids_col == eid_col[:, 1:2]
    after = jnp.where(second < first, 1.0, 0.0).astype(BF16)
    slot = mm(after, jnp.where(is0 | is1, 1.0, 0.0).astype(BF16)) + (cap * ids_col).astype(F32)
    places = lax.broadcasted_iota(jnp.int32, (rows, pick0.shape[1]), 1).astype(F32)
    for pick, chosen in ((pick0, is0), (pick1, is1)):
        where_to = jnp.sum(jnp.where(chosen, slot, 0.0), axis=1, keepdims=True)
        pick[...] = jnp.where(places == where_to, 1.0, 0.0).astype(BF16)

    loads[0].wait()
    step_rows = 16

    def norm_step(n, carry):
        at = pl.ds(pl.multiple_of(n * step_rows, step_rows), step_rows)
        features = x[at, :].astype(F32)
        centred = features - jnp.mean(features, -1, keepdims=True)
        spread = lax.rsqrt(jnp.mean(centred * centred, -1, keepdims=True) + NORM_EPS)
        normed[at, :] = (centred * spread * gain[...]).astype(BF16)
        return carry

    lax.fori_loop(0, rows // step_rows, norm_step, 0)
    pl.semaphore_wait(barrier, ep_size + 2)

    def dispatch_copy(k, m):
        return pltpu.make_async_remote_copy(
            send_buf.at[k, m], arrived.at[core, k, m], disp_send.at[k, m], disp_recv.at[k, m],
            device_id={"ep": target(k, m)},
        )

    def forward_copy(k, m):
        return pltpu.make_async_remote_copy(
            arrived.at[core, k, m], arrived.at[core, k, m], fwd_send.at[k, m], fwd_recv.at[k, m],
            device_id={"tp_1": 1 - core},
        )

    places_row = lax.broadcasted_iota(jnp.int32, (cap, rows), 0).astype(F32)

    def gather_group(k, carry):
        picks = [
            jnp.where(
                rank_row[pl.ds(2 * target(k, m) + core, 1), :] == places_row, 1.0, 0.0
            ).astype(BF16)
            for m in range(side)
        ]
        sel = jnp.concatenate(picks, 0)
        for n in range(0, width, 512):
            got = mm(sel, normed[:, n : n + 512]).astype(BF16)
            send_buf[k, :, :, n : n + 512] = got.reshape(side, cap, 512)
        for m in range(side):
            if m == 0:
                @pl.when(k == 0)
                def _():
                    arrived[core, 0, 0] = send_buf[0, 0]

                @pl.when(k > 0)
                def _():
                    dispatch_copy(k, m).start()
            else:
                dispatch_copy(k, m).start()
        return carry

    lax.fori_loop(0, side, gather_group, 0)
    for load in loads[1:]:
        load.wait()

    def ring_length(h, f):
        return zs // 2 if h == f else zs // 2 - 1

    def half(h):
        return pl.ds(h * group_rows, group_rows)

    def neighbour(f):
        return (z + 1) % zs if f == 0 else (z + zs - 1) % zs

    def ring_copy(k, h, f, s):
        length = ring_length(h, f)
        toward = (z + length) % zs if f == 0 else (z + zs - length) % zs
        origin = partial.at[k, toward, core, half(h)] if s == 0 else ring_buf.at[k, h, f, s - 1]
        return pltpu.make_async_remote_copy(
            origin, ring_buf.at[k, h, f, s], ring_send.at[k, h, f, s], ring_recv.at[k, h, f, s],
            device_id={"tp_0": neighbour(f)},
        )

    def ring_step(k, s):
        for h, f in RINGS:
            length = ring_length(h, f)
            if s >= length:
                continue
            if s > 0:
                ring_copy(k, h, f, s - 1).wait_recv()
                left = length - s
                toward = (z + left) % zs if f == 0 else (z + zs - left) % zs
                ring_buf[k, h, f, s - 1] = (
                    ring_buf[k, h, f, s - 1].astype(F32)
                    + partial[k, toward, core, half(h)].astype(F32)
                ).astype(BF16)
            ring_copy(k, h, f, s).start()

    def pair_copy(k):
        return pltpu.make_async_remote_copy(
            partial.at[k, :, 1 - core], pair_buf.at[k], pair_send.at[k], pair_recv.at[k],
            device_id={"tp_1": 1 - core},
        )

    def return_copy(k, m):
        return pltpu.make_async_remote_copy(
            final_buf.at[k, :, m], ret.at[me], ret_send.at[k, m], ret_recv.at[me],
            device_id={"ep": source(k, m)},
        )

    def finish(k):
        for h in range(2):
            lengths = [ring_length(h, f) for f in range(2)]
            for f in range(2):
                ring_copy(k, h, f, lengths[f] - 1).wait_recv()
            total = (
                partial[k, z, core, half(h)].astype(F32)
                + ring_buf[k, h, 0, lengths[0] - 1].astype(F32)
                + ring_buf[k, h, 1, lengths[1] - 1].astype(F32)
            )
            final_buf[k, h] = total.astype(BF16).reshape(final_buf.shape[2:])
        for m in range(side):
            if m == 0:
                @pl.when(k == 0)
                def _():
                    ret[me] = final_buf[0, :, 0]

                @pl.when(k > 0)
                def _():
                    return_copy(k, m).start()
            else:
                return_copy(k, m).start()

    def take_pair(k):
        pair_copy(k).wait_recv()
        for d in range(zs):
            partial[k, d, core] = (
                partial[k, d, core].astype(F32) + pair_buf[k, d].astype(F32)
            ).astype(BF16)

    def compute(k):
        for q in range(2):
            tokens = arrived[q, k].reshape(group_rows, width)
            gate = mm(tokens, wg[q])
            up = mm(tokens, wu[q])
            hidden = (jax.nn.silu(gate) * up).astype(BF16)
            for n in range(0, width, 512):
                part = mm(hidden, wd[q, :, n : n + 512]).astype(BF16)
                for i in range(4):
                    s = n // 128 + i
                    partial[k, s // 2, s % 2, half(q)] = part[:, 128 * i : 128 * i + 128]

    def group_step(k, carry):
        for m in range(side):
            if m == 0:
                @pl.when(k > 0)
                def _():
                    dispatch_copy(k, 0).wait_recv()
            else:
                dispatch_copy(k, m).wait_recv()
            forward_copy(k, m).start()

            @pl.when(k > 0)
            def _():
                ring_step(k - 1, m)

        for m in range(side):
            forward_copy(k, m).wait_recv()
        compute(k)
        pair_copy(k).start()

        @pl.when(k > 0)
        def _():
            finish(k - 1)

        take_pair(k)
        return carry

    lax.fori_loop(0, side, group_step, 0)
    for s in range(side):
        ring_step(side - 1, s)
    finish(side - 1)

    def take_returns(k, carry):
        for m in range(side):
            def wait_one():
                there = target(k, m)
                pltpu.make_async_remote_copy(
                    final_buf.at[k, :, m], ret.at[there], ret_send.at[k, m], ret_recv.at[there],
                    device_id={"ep": there},
                ).wait_recv()

            if m == 0:
                pl.when(k > 0)(wait_one)
            else:
                wait_one()
        return carry

    lax.fori_loop(0, side, take_returns, 0)
    copies = ret[...].reshape(pick0.shape[1], 128)
    out[...] = (
        weight_col[:, 0:1] * mm(pick0[...], copies) + weight_col[:, 1:2] * mm(pick1[...], copies)
    ).astype(BF16)

    def drain(k, carry):
        for m in range(side):
            def sent():
                dispatch_copy(k, m).wait_send()
                return_copy(k, m).wait_send()

            if m == 0:
                pl.when(k > 0)(sent)
            else:
                sent()
            forward_copy(k, m).wait_send()
        pair_copy(k).wait_send()
        for h, f in RINGS:
            for s in range(ring_length(h, f)):
                ring_copy(k, h, f, s).wait_send()
        return carry

    lax.fori_loop(0, side, drain, 0)


def expert_side(x, gain, eid_row, eid_col, weight_col, wg, wu, wd):
    rows, width = x.shape
    ep_size, zs = lax.axis_size("ep"), lax.axis_size("tp_0")
    side = int(round(ep_size**0.5))
    experts = 2 * ep_size
    cap = 2 * rows // experts
    group_rows = side * cap
    ring_slots = zs // 2
    dma = pltpu.SemaphoreType.DMA
    vmem = pl.BlockSpec(memory_space=pltpu.VMEM)
    hbm = pl.BlockSpec(memory_space=pl.ANY)
    return pl.pallas_call(
        expert_kernel,
        out_shape=jax.ShapeDtypeStruct((rows, width // (2 * zs)), BF16),
        in_specs=[hbm, vmem, vmem, vmem, vmem, hbm, hbm, hbm],
        out_specs=vmem,
        scratch_shapes=[
            pltpu.VMEM(x.shape, BF16),
            pltpu.VMEM(x.shape, BF16),
            pltpu.VMEM(wg.shape, BF16),
            pltpu.VMEM(wu.shape, BF16),
            pltpu.VMEM(wd.shape, BF16),
            pltpu.VMEM((experts, rows), F32),
            pltpu.VMEM((side, side, cap, width), BF16),
            pltpu.VMEM((2, side, side, cap, width), BF16),
            pltpu.VMEM((side, zs, 2, 2 * group_rows, 128), BF16),
            pltpu.VMEM((side, zs, 2 * group_rows, 128), BF16),
            pltpu.VMEM((side, 2, 2, ring_slots, group_rows, 128), BF16),
            pltpu.VMEM((side, 2, side, cap, 128), BF16),
            pltpu.VMEM((ep_size, 2, cap, 128), BF16),
            pltpu.VMEM((rows, experts * cap), BF16),
            pltpu.VMEM((rows, experts * cap), BF16),
            dma((4,)),
            dma((side, side)), dma((side, side)),
            dma((side, side)), dma((side, side)),
            dma((side,)), dma((side,)),
            dma((side, 2, 2, ring_slots)), dma((side, 2, 2, ring_slots)),
            dma((side, side)), dma((ep_size,)),
        ],
        compiler_params=pltpu.CompilerParams(
            collective_id=0, has_side_effects=True, vmem_limit_bytes=60 * 1024 * 1024
        ),
        cost_estimate=pl.CostEstimate(
            flops=40_000_000_000, bytes_accessed=20_000_000, transcendentals=0
        ),
        name="expert_side",
    )(x, gain, eid_row, eid_col, weight_col, wg, wu, wd)


def on_device(
    queries,
    values,
    forget_gate_logits,
    output_gate_logits,
    forget_gate_headroom,
    spike_log_decay,
    head_norm_gain,
    output_projection,
    second_micro_input,
    expert_norm_gain,
    token_group_index,
    token_expert_pair,
    group_router_scores,
    expert_router_scores,
    expert_gate_weight,
    expert_up_weight,
    expert_down_weight,
):
    row_count = queries.shape[0]
    head_count = forget_gate_headroom.shape[1] // HEAD_DIM
    block_count = row_count // BLOCK
    logarithm_decay, key_contributions = decay_pieces(
        forget_gate_logits, forget_gate_headroom, spike_log_decay
    )
    lifted = jax.nn.silu(queries.astype(jnp.float32))
    inputs_f = values.astype(jnp.float32)

    def directed(tensor):
        both = jnp.stack([tensor[0], jnp.flip(tensor[1], 0)])
        return both.reshape(2, block_count, BLOCK, head_count, HEAD_DIM)

    query_dir = directed(jnp.stack([lifted, lifted]))
    value_dir = directed(jnp.stack([inputs_f, inputs_f]))
    key_dir = directed(key_contributions)
    running_state = jnp.cumsum(directed(logarithm_decay), axis=2)
    final_block_row = running_state[:, :, -1:]
    query_up = query_dir * jnp.exp(running_state - final_block_row)
    key_down = key_dir * jnp.exp(final_block_row - running_state)
    scores = jnp.einsum("nbthk,nbshk->nbhts", query_up, key_down)
    causal = jnp.tril(jnp.ones((BLOCK, BLOCK), bool))
    scores = jnp.where(causal, scores, 0.0)
    inner_out = jnp.einsum("nbhts,nbshv->nbthv", scores, value_dir)
    block_states = jnp.einsum("nbshk,nbshv->nbhkv", key_down, value_dir)
    block_decay = final_block_row[:, :, 0]
    through = jnp.cumsum(block_decay, axis=1)
    entry_sum = through - block_decay
    block_ids = jnp.arange(block_count)
    earlier_mask = (block_ids[None, :] < block_ids[:, None])[None, :, :, None, None]
    between = entry_sum[:, :, None] - through[:, None, :]
    carry_wts = jnp.where(earlier_mask, jnp.exp(jnp.where(earlier_mask, between, 0.0)), 0.0)
    local_entry = jnp.einsum("nbchk,nchkv->nbhkv", carry_wts, block_states)
    device_decay = through[:, -1]
    tail_wts = jnp.exp(device_decay[:, None] - through)
    device_state = jnp.einsum("nchk,nchkv->nhkv", tail_wts, block_states)
    zero_decay = jnp.zeros_like(device_decay[0])
    zero_state = jnp.zeros_like(device_state[0])
    forward_pair = prefix(
        (device_decay[0], device_state[0]), "ep", combine_states, (zero_decay, zero_state), False
    )
    backward_pair = prefix(
        (device_decay[1], device_state[1]), "ep", combine_states, (zero_decay, zero_state), True
    )
    incoming = jnp.stack([forward_pair[1], backward_pair[1]])
    block_entry = local_entry + jnp.exp(entry_sum)[..., None] * incoming[:, None]
    across_block_output = jnp.einsum(
        "nbthk,nbhkv->nbthv", query_dir * jnp.exp(running_state), block_entry
    )
    direction_out = (across_block_output + inner_out).reshape(2, row_count, head_count, HEAD_DIM)
    joined = direction_out[0] + jnp.flip(direction_out[1], 0)
    normed = joined * lax.rsqrt(jnp.mean(joined * joined, -1, keepdims=True) + HEAD_EPS)
    readout = (
        normed.reshape(row_count, -1)
        * head_norm_gain
        * jax.nn.silu(output_gate_logits.astype(jnp.float32))
    ).astype(jnp.bfloat16)
    mixed_sum = jnp.dot(
        lax.all_gather(readout, TP, axis=1, tiled=True),
        output_projection,
        preferred_element_type=jnp.float32,
    )
    recurrence_output = mixed_sum.astype(jnp.bfloat16)
    group_count = group_router_scores.shape[1]
    group_prob = jax.nn.softmax(group_router_scores, axis=-1)
    chosen = jnp.sum(
        jnp.where(jnp.arange(group_count)[None, :] == token_group_index[:, None], group_prob, 0.0),
        -1,
    )
    pair_weight = (
        jnp.stack(
            [
                jax.nn.sigmoid(expert_router_scores[:, 0] - expert_router_scores[:, 1]),
                jax.nn.sigmoid(expert_router_scores[:, 1] - expert_router_scores[:, 0]),
            ],
            -1,
        )
        * chosen[:, None]
    )
    expert_id = token_group_index[:, None] * GROUP_EXP + token_expert_pair
    expert_tokens = expert_side(
        second_micro_input,
        expert_norm_gain[None, :],
        expert_id.T,
        expert_id,
        pair_weight,
        expert_gate_weight,
        expert_up_weight,
        expert_down_weight,
    )
    return (recurrence_output, expert_tokens)


def solution(mesh):
    split = Mesh(mesh.devices.reshape(mesh.shape["ep"], 8, 2), ("ep", "tp_0", "tp_1"))
    placed = (
        P("ep", TP),
        P("ep", TP),
        P(None, "ep", TP),
        P("ep", TP),
        P(None, TP),
        P("ep"),
        P(TP),
        P(None, TP),
        P("ep", None),
        P(),
        P("ep"),
        P("ep", None),
        P("ep", None),
        P("ep", None),
        P("ep", None, TP),
        P("ep", None, TP),
        P("ep", TP, None),
    )
    return jax.shard_map(
        on_device,
        mesh=split,
        in_specs=placed,
        out_specs=(P("ep", TP), P("ep", TP)),
        check_vma=False,
    )
```

```python
import jax
import jax.numpy as jnp
from jax import lax
from jax.experimental import pallas as pl
from jax.experimental.pallas import tpu as pltpu
from jax.sharding import Mesh
from jax.sharding import PartitionSpec as P

GROUP_EXP = 4
BLOCK = 64
TP = ("tp_0", "tp_1")


HEAD_EPS = 1e-06
NORM_EPS = 1e-05


F32, BF16 = jnp.float32, jnp.bfloat16
RINGS = ((0, 0), (0, 1), (1, 0), (1, 1))


def mm(a, b):
    return jnp.dot(a, b, preferred_element_type=F32)


def dot_last(a, b):
    return lax.dot_general(a, b, (((1,), (1,)), ((), ())), preferred_element_type=F32)


def thirds(value):
    high = value.astype(BF16)
    rest = value - high.astype(F32)
    middle = rest.astype(BF16)
    return high, middle, (rest - middle.astype(F32)).astype(BF16)


def whole_kernel(
    x_hbm, gain, group_index, pair, group_scores, pair_scores, wg_hbm, wu_hbm, wd_hbm,
    queries, values, logits, gates, headroom, spike, head_gain, proj_hbm,
    rec_out, out,
    x, normed, wg, wu, wd, rank_row, send_buf, arrived, partial, pair_buf,
    ring_buf, final_buf, ret, pick0, pick1,
    proj, cum, joined, block_state, block_total, entry_state, entry_sum, decayed,
    state_send, states, incoming, readout, columns,
    load_sem, disp_send, disp_recv, fwd_send, fwd_recv, pair_send, pair_recv,
    ring_send, ring_recv, ret_send, ret_recv,
    state_ssem, state_rsem, read_send, read_recv, side_send, side_recv,
):
    side = arrived.shape[1]
    cap = arrived.shape[3]
    zs = partial.shape[1]
    rows, width = x.shape
    group_rows = side * cap
    ep_size = side * side
    experts = 2 * ep_size
    me, z, core = lax.axis_index("ep"), lax.axis_index("tp_0"), lax.axis_index("tp_1")
    my_y, my_x = me // side, me % side
    loads = [
        pltpu.make_async_copy(a, b, load_sem.at[n])
        for n, (a, b) in enumerate((
            (x_hbm, x), (wg_hbm, wg), (wu_hbm, wu), (wd_hbm, wd), (proj_hbm, proj)
        ))
    ]
    loads[0].start()

    barrier = pltpu.get_barrier_semaphore()

    def greet(n, carry):
        pl.semaphore_signal(barrier, 1, device_id={"ep": (me + n) % ep_size})
        return carry

    lax.fori_loop(1, ep_size, greet, 0)
    pl.semaphore_signal(barrier, 1, device_id={"tp_1": 1 - core})
    pl.semaphore_signal(barrier, 1, device_id={"tp_0": (z + 1) % zs})
    pl.semaphore_signal(barrier, 1, device_id={"tp_0": (z + zs - 1) % zs})

    def target(k, m):
        return ((my_y + 2 * side - (m + k) % side) % side) * side + (my_x + side - m) % side

    def source(k, m):
        return ((my_y + (m + k) % side) % side) * side + (my_x + m) % side

    first = lax.broadcasted_iota(jnp.int32, (rows, rows), 0)
    second = lax.broadcasted_iota(jnp.int32, (rows, rows), 1)
    ids = lax.broadcasted_iota(jnp.int32, (experts, rows), 0)
    group = group_index[...].reshape(1, rows)
    chosen = [ids == group * GROUP_EXP + pair[n : n + 1, :] for n in range(2)]
    named = chosen[0] | chosen[1]
    before = jnp.where(first < second, 1.0, 0.0).astype(BF16)
    rank = mm(jnp.where(named, 1.0, 0.0).astype(BF16), before)
    rank_row[...] = jnp.where(named, rank, -1.0)
    away_y = (my_y + side - ids // (2 * side)) % side
    away_x = (my_x + side - ids // 2 % side) % side
    step_of = (away_y + side - away_x) % side
    slot = rank + (cap * ((step_of * side + away_x) * 2 + ids % 2)).astype(F32)
    powers = jnp.exp(group_scores[...] - jnp.max(group_scores[...], axis=0, keepdims=True))
    groups = lax.broadcasted_iota(jnp.int32, powers.shape, 0)
    share = jnp.sum(jnp.where(groups == group, powers, 0.0), axis=0, keepdims=True) / jnp.sum(
        powers, axis=0, keepdims=True
    )
    lead = pair_scores[0:1, :] - pair_scores[1:2, :]
    lines = [jnp.sum(jnp.where(which, slot, 0.0), axis=0, keepdims=True) for which in chosen]
    lines += [share * jax.nn.sigmoid(lead), share * jax.nn.sigmoid(-lead), spike[...].reshape(1, rows)]
    columns[...] = jnp.concatenate(lines + [jnp.zeros((3, rows), F32)], 0).T
    wide = 4 * BLOCK
    blocks = rows // BLOCK
    at_row = lax.broadcasted_iota(jnp.int32, (wide, wide), 0)
    at_col = lax.broadcasted_iota(jnp.int32, (wide, wide), 1)
    same = at_row // BLOCK == at_col // BLOCK
    reach = (same & (at_col <= at_row), same & (at_col >= at_row))
    block_of = lax.broadcasted_iota(jnp.int32, (wide, 128), 0) // BLOCK

    def local_part(g, carry):
        at = pl.ds(pl.multiple_of(g * wide, wide), wide)
        lifted = jax.nn.silu(queries[at, :].astype(F32))
        inputs = values[at, :]
        inputs_t = inputs.astype(F32).T.astype(BF16)
        scores = jnp.zeros((wide, wide), F32)
        for d in range(2):
            keys = headroom[d : d + 1, :] * jax.nn.sigmoid(-logits[d, at, :].astype(F32))
            decay = jnp.log1p(-keys) + columns[at, 4:5]
            sums = mm(
                jnp.where(reach[d], 1.0, 0.0).astype(BF16), jnp.concatenate(thirds(decay), 1)
            )
            run = sums[:, :128] + sums[:, 128:256] + sums[:, 256:]
            cum[d, at, :] = run
            run4 = run.reshape(4, BLOCK, 128)
            middle = run4[:, BLOCK // 2 : BLOCK // 2 + 1]
            last = run4[:, BLOCK - 1 :] if d == 0 else run4[:, :1]
            over = (run4 - middle).reshape(wide, 128)
            left = (last - run4).reshape(wide, 128)
            found = dot_last(
                (lifted * jnp.exp(over)).astype(BF16), (keys * jnp.exp(-over)).astype(BF16)
            )
            scores = scores + jnp.where(reach[d], found, 0.0)
            written = keys * jnp.exp(left)
            spread = jnp.concatenate(
                [jnp.where(block_of == b, written, 0.0).astype(BF16) for b in range(4)], 1
            )
            state = mm(inputs_t, spread)
            for b in range(4):
                block_state[d, 4 * g + b] = state[:, 128 * b : 128 * b + 128]
                block_total[d, 4 * g + b] = last[b]
            decayed[at, 128 * d : 128 * d + 128] = (lifted * jnp.exp(run)).astype(BF16)
        joined[at, :] = mm(scores.astype(BF16), inputs)
        return carry

    lax.fori_loop(0, rows // wide, local_part, 0)

    line = lax.broadcasted_iota(jnp.int32, (16, 128), 0)
    for d in range(2):
        def advance(n, carry, d=d):
            state, total = carry
            b = n if d == 0 else blocks - 1 - n
            entry_state[b, :, 128 * d : 128 * d + 128] = state.astype(BF16)
            entry_sum[d, b] = total
            own = block_total[d, b]
            return jnp.exp(own) * state + block_state[d, b], total + own

        state, total = lax.fori_loop(
            0, blocks, advance, (jnp.zeros((128, 128), F32), jnp.zeros((1, 128), F32))
        )
        state_send[d, :128] = state.astype(BF16)
        terms = jnp.zeros((16, 128), F32)
        for n, term in enumerate(thirds(total)):
            terms = jnp.where(line == n, term.astype(F32), terms)
        state_send[d, 128:] = terms.astype(BF16)

    pl.semaphore_wait(barrier, ep_size + 2)

    def state_copy(n):
        there = (me + n) % ep_size
        return pltpu.make_async_remote_copy(
            state_send.at[1 - (there + ep_size - me) // ep_size], states.at[me],
            state_ssem.at[n], state_rsem.at[me], device_id={"ep": there},
        )

    def state_start(n, carry):
        state_copy(n).start()
        return carry

    lax.fori_loop(1, ep_size, state_start, 0)

    def state_sent(n, carry):
        state_copy(n).wait_send()
        return carry

    loads[0].wait()
    for load in loads[1:]:
        load.start()
    step_rows = rows // 8

    def norm_step(n, carry):
        at = pl.ds(pl.multiple_of(n * step_rows, step_rows), step_rows)
        features = x[at, :].astype(F32)
        centred = features - jnp.mean(features, -1, keepdims=True)
        spread = lax.rsqrt(jnp.mean(centred * centred, -1, keepdims=True) + NORM_EPS)
        normed[at, :] = (centred * spread * gain[...]).astype(BF16)
        return carry

    lax.fori_loop(0, rows // step_rows, norm_step, 0)

    def dispatch_copy(k, m):
        return pltpu.make_async_remote_copy(
            send_buf.at[k, m], arrived.at[core, k, m], disp_send.at[k, m], disp_recv.at[k, m],
            device_id={"ep": target(k, m)},
        )

    def forward_copy(k, m):
        return pltpu.make_async_remote_copy(
            arrived.at[core, k, m], arrived.at[core, k, m], fwd_send.at[k, m], fwd_recv.at[k, m],
            device_id={"tp_1": 1 - core},
        )

    def dispatch_start(k, m, n):
        lanes = slice(n * width // 2, (n + 1) * width // 2)
        pltpu.make_async_remote_copy(
            send_buf.at[k, m, :, lanes], arrived.at[core, k, m, :, lanes],
            disp_send.at[k, m], disp_recv.at[k, m], device_id={"ep": target(k, m)},
        ).start()

    def dispatch_group(k):
        for n in range(2):
            for m in range(side):
                if m == 0:
                    pl.when(k > 0)(lambda n=n: dispatch_start(k, 0, n))
                else:
                    dispatch_start(k, m, n)

    places_row = lax.broadcasted_iota(jnp.int32, (cap, rows), 0).astype(F32)

    def selection(k):
        picks = [
            jnp.where(
                rank_row[pl.ds(2 * target(k, m) + core, 1), :] == places_row, 1.0, 0.0
            ).astype(BF16)
            for m in range(side)
        ]
        return jnp.concatenate(picks, 0)

    def gather_group(k):
        sel = selection(k)
        for n in range(2):
            for at in range(n * width // 2, (n + 1) * width // 2, 512):
                got = mm(sel, normed[:, at : at + 512]).astype(BF16)
                send_buf[k, :, :, at : at + 512] = got.reshape(side, cap, 512)

        @pl.when(k == 0)
        def _():
            arrived[core, 0, 0] = send_buf[0, 0]

        pl.when(k < 2)(lambda: dispatch_group(k))

    lax.fori_loop(1, ep_size, state_sent, 0)

    def gather_whole(k, carry):
        gather_group(k)
        return carry

    lax.fori_loop(0, side, gather_whole, 0)

    def across(b, carry):
        at = pl.ds(pl.multiple_of(b * BLOCK, BLOCK), BLOCK)
        joined[at, :] += dot_last(decayed[at, :], entry_state[b])
        lifted = jax.nn.silu(queries[at, :].astype(F32))
        for d in range(2):
            decayed[at, 128 * d : 128 * d + 128] = (
                lifted * jnp.exp(cum[d, at, :] + entry_sum[d, b])
            ).astype(BF16)
        return carry

    lax.fori_loop(0, blocks, across, 0)

    places = lax.broadcasted_iota(jnp.int32, pick0.shape, 1).astype(F32)
    for n, pick in enumerate((pick0, pick1)):
        pick[...] = jnp.where(places == columns[:, n : n + 1], 1.0, 0.0).astype(BF16)

    for load in loads[1:]:
        load.wait()

    def read_slice(chip, which):
        return pl.ds(pl.multiple_of((2 * chip + which) * 128, 128), 128)

    def read_copy(f, s):
        chip = (z + zs - s) % zs if f == 0 else (z + s) % zs
        lines = pl.ds(0, rows) if s < zs // 2 - 1 else pl.ds(f * (rows // 2), rows // 2)
        piece = readout.at[lines, read_slice(chip, core)]
        return pltpu.make_async_remote_copy(
            piece, piece, read_send.at[f, s], read_recv.at[f, s],
            device_id={"tp_0": (z + 1) % zs if f == 0 else (z + zs - 1) % zs},
        )

    def side_copy(distance):
        piece = readout.at[:, read_slice((z + distance) % zs, core)]
        return pltpu.make_async_remote_copy(
            piece, piece, side_send.at[distance], side_recv.at[distance],
            device_id={"tp_1": 1 - core},
        )

    def read_step(s):
        for f in range(2):
            if s > 0:
                read_copy(f, s - 1).wait_recv()
            if s < zs // 2:
                read_copy(f, s).start()
        for distance in {s % zs, (zs - s) % zs}:
            side_copy(distance).start()

    def finish_readout():
        for d in range(2):
            lanes = slice(128 * d, 128 * d + 128)

            def one(n, state, d=d):
                source_at = n if d == 0 else ep_size - 1 - n
                used = source_at < me if d == 0 else source_at > me

                def taken(state):
                    pltpu.make_async_remote_copy(
                        state_send.at[0], states.at[source_at], state_ssem.at[0],
                        state_rsem.at[source_at], device_id={"ep": source_at},
                    ).wait_recv()
                    got = states[source_at].astype(F32)
                    total = jnp.sum(got[128:], axis=0, keepdims=True)
                    return jnp.exp(total) * state + got[:128]

                return lax.cond(used, taken, lambda state: state, state)

            state = lax.fori_loop(0, ep_size, one, jnp.zeros((128, 128), F32))
            incoming[:, lanes] = state.astype(BF16)

        def settle(g, carry):
            at = pl.ds(pl.multiple_of(g * wide, wide), wide)
            total = joined[at, :] + dot_last(decayed[at, :], incoming[...])
            scale = lax.rsqrt(jnp.mean(total * total, -1, keepdims=True) + HEAD_EPS)
            gate = jax.nn.silu(gates[at, :].astype(F32))
            readout[at, read_slice(z, core)] = (total * scale * head_gain[...] * gate).astype(BF16)
            return carry

        lax.fori_loop(0, rows // wide, settle, 0)
        read_step(0)

    def ring_length(h, f):
        return zs // 2 if h == f else zs // 2 - 1

    def half(h):
        return pl.ds(h * group_rows, group_rows)

    def neighbour(f):
        return (z + 1) % zs if f == 0 else (z + zs - 1) % zs

    def ring_copy(k, h, f, s):
        length = ring_length(h, f)
        toward = (z + length) % zs if f == 0 else (z + zs - length) % zs
        origin = partial.at[k, toward, core, half(h)] if s == 0 else ring_buf.at[k, h, f, s - 1]
        return pltpu.make_async_remote_copy(
            origin, ring_buf.at[k, h, f, s], ring_send.at[k, h, f, s], ring_recv.at[k, h, f, s],
            device_id={"tp_0": neighbour(f)},
        )

    def ring_step(k, s, only=None):
        for h, f in RINGS:
            length = ring_length(h, f)
            if s >= length or only not in (None, h):
                continue
            if s > 0:
                ring_copy(k, h, f, s - 1).wait_recv()
                left = length - s
                toward = (z + left) % zs if f == 0 else (z + zs - left) % zs
                ring_buf[k, h, f, s - 1] = (
                    ring_buf[k, h, f, s - 1].astype(F32)
                    + partial[k, toward, core, half(h)].astype(F32)
                ).astype(BF16)
            ring_copy(k, h, f, s).start()

    def pair_copy(k, q):
        return pltpu.make_async_remote_copy(
            partial.at[k, :, 1 - core, half(q)], pair_buf.at[k, :, half(q)],
            pair_send.at[k, q], pair_recv.at[k, q], device_id={"tp_1": 1 - core},
        )

    def return_copy(k, m):
        return pltpu.make_async_remote_copy(
            final_buf.at[k, :, m], ret.at[k, m], ret_send.at[k, m], ret_recv.at[k, m],
            device_id={"ep": source(k, m)},
        )

    def finish(k):
        for h in range(2):
            lengths = [ring_length(h, f) for f in range(2)]
            for f in range(2):
                ring_copy(k, h, f, lengths[f] - 1).wait_recv()
            total = (
                partial[k, z, core, half(h)].astype(F32)
                + ring_buf[k, h, 0, lengths[0] - 1].astype(F32)
                + ring_buf[k, h, 1, lengths[1] - 1].astype(F32)
            )
            final_buf[k, h] = total.astype(BF16).reshape(final_buf.shape[2:])
        for m in range(side):
            if m == 0:
                @pl.when(k == 0)
                def _():
                    ret[0, 0] = final_buf[0, :, 0]

                @pl.when(k > 0)
                def _():
                    return_copy(k, m).start()
            else:
                return_copy(k, m).start()

    def take_pair(k, q):
        pair_copy(k, q).wait_recv()
        for d in range(zs):
            partial[k, d, core, half(q)] = (
                partial[k, d, core, half(q)].astype(F32) + pair_buf[k, d, half(q)].astype(F32)
            ).astype(BF16)
        ring_step(k, 0, q)

    def compute(k):
        for q in range(2):
            tokens = arrived[q, k].reshape(group_rows, width)
            gate = mm(tokens, wg[q])
            up = mm(tokens, wu[q])
            hidden = (jax.nn.silu(gate) * up).astype(BF16)
            for n in range(0, width, 512):
                part = mm(hidden, wd[q, :, n : n + 512]).astype(BF16)
                for i in range(4):
                    s = n // 128 + i
                    partial[k, s // 2, s % 2, half(q)] = part[:, 128 * i : 128 * i + 128]
            pair_copy(k, q).start()

    def group_step(k, carry):
        pl.when(k == 0)(lambda: read_step(1))
        for m in range(side):
            if m == 0:
                pl.when(k > 0)(lambda: dispatch_copy(k, 0).wait_send())
            else:
                dispatch_copy(k, m).wait_send()
        pl.when(k < side - 2)(lambda: dispatch_group(k + 2))
        for m in range(side):
            if m == 0:
                pl.when(k > 0)(lambda: dispatch_copy(k, 0).wait_recv())
            else:
                dispatch_copy(k, m).wait_recv()
            forward_copy(k, m).start()

        for n in range(1, side):
            pl.when(k >= n)(lambda n=n: ring_step(k - n, n))
        for m in range(side):
            forward_copy(k, m).wait_recv()
        compute(k)
        for q in range(2):
            take_pair(k, q)

        for n in range(2, side + 1):
            pl.when(k == n - 2)(lambda n=n: read_step(n))
        return carry

    finish_readout()
    lax.fori_loop(0, side, group_step, 0)
    final = side - 1
    ring_step(final, 1)
    ring_step(final - 1, 2)
    ring_step(final - 2, 3)
    finish(final - 3)
    ring_step(final, 2)
    ring_step(final - 1, 3)
    finish(final - 2)
    for distance in range(zs):
        side_copy(distance).wait_recv()
    rec_out[...] = mm(readout[...], proj[...])
    ring_step(final, 3)
    finish(final - 1)

    def take_returns(k, carry):
        for m in range(side):
            if m == 0:
                pl.when(k > 0)(lambda: return_copy(k, 0).wait_recv())
            else:
                return_copy(k, m).wait_recv()
        return carry

    def combined(k, count):
        copies = ret[k : k + count].reshape(count * 2 * group_rows, 128)
        lanes = slice(k * 2 * group_rows, (k + count) * 2 * group_rows)
        return columns[:, 2:3] * mm(pick0[:, lanes], copies) + columns[:, 3:4] * mm(
            pick1[:, lanes], copies
        )

    lax.fori_loop(0, final, take_returns, 0)
    out[...] = combined(0, final)
    finish(final)
    take_returns(final, 0)
    out[...] += combined(final, 1)

    def drain(k, carry):
        for m in range(side):
            def sent():
                return_copy(k, m).wait_send()

            if m == 0:
                pl.when(k > 0)(sent)
            else:
                sent()
            forward_copy(k, m).wait_send()
        for q in range(2):
            pair_copy(k, q).wait_send()
        for h, f in RINGS:
            for s in range(ring_length(h, f)):
                ring_copy(k, h, f, s).wait_send()
        return carry

    lax.fori_loop(0, side, drain, 0)

    for s in range(zs // 2):
        for f in range(2):
            read_copy(f, s).wait_send()
    for distance in range(zs):
        side_copy(distance).wait_send()


def on_device(
    queries,
    values,
    forget_gate_logits,
    output_gate_logits,
    forget_gate_headroom,
    spike_log_decay,
    head_norm_gain,
    output_projection,
    second_micro_input,
    expert_norm_gain,
    token_group_index,
    token_expert_pair,
    group_router_scores,
    expert_router_scores,
    expert_gate_weight,
    expert_up_weight,
    expert_down_weight,
):
    rows, width = second_micro_input.shape
    ep_size, zs = lax.axis_size("ep"), lax.axis_size("tp_0")
    side = int(round(ep_size**0.5))
    experts = 2 * ep_size
    cap = 2 * rows // experts
    group_rows = side * cap
    ring_slots = zs // 2
    blocks = rows // BLOCK
    dma = pltpu.SemaphoreType.DMA
    vmem = pl.BlockSpec(memory_space=pltpu.VMEM)
    hbm = pl.BlockSpec(memory_space=pl.ANY)
    result = jax.ShapeDtypeStruct((rows, 128), F32)
    results = pl.pallas_call(
        whole_kernel,
        out_shape=(result, result),
        in_specs=[hbm, vmem, vmem, vmem, vmem, vmem, hbm, hbm, hbm]
        + [vmem, vmem, vmem, vmem, vmem, vmem, vmem, hbm],
        out_specs=(vmem, vmem),
        scratch_shapes=[
            pltpu.VMEM((rows, width), BF16),
            pltpu.VMEM((rows, width), BF16),
            pltpu.VMEM(expert_gate_weight.shape, BF16),
            pltpu.VMEM(expert_up_weight.shape, BF16),
            pltpu.VMEM(expert_down_weight.shape, BF16),
            pltpu.VMEM((experts, rows), F32),
            pltpu.VMEM((side, side, cap, width), BF16),
            pltpu.VMEM((2, side, side, cap, width), BF16),
            pltpu.VMEM((side, zs, 2, 2 * group_rows, 128), BF16),
            pltpu.VMEM((side, zs, 2 * group_rows, 128), BF16),
            pltpu.VMEM((side, 2, 2, ring_slots, group_rows, 128), BF16),
            pltpu.VMEM((side, 2, side, cap, 128), BF16),
            pltpu.VMEM((side, side, 2, cap, 128), BF16),
            pltpu.VMEM((rows, experts * cap), BF16),
            pltpu.VMEM((rows, experts * cap), BF16),
            pltpu.VMEM(output_projection.shape, BF16),
            pltpu.VMEM((2, rows, 128), F32),
            pltpu.VMEM((rows, 128), F32),
            pltpu.VMEM((2, blocks, 128, 128), F32),
            pltpu.VMEM((2, blocks, 1, 128), F32),
            pltpu.VMEM((blocks, 128, 256), BF16),
            pltpu.VMEM((2, blocks, 1, 128), F32),
            pltpu.VMEM((rows, 256), BF16),
            pltpu.VMEM((2, 144, 128), BF16),
            pltpu.VMEM((ep_size, 144, 128), BF16),
            pltpu.VMEM((128, 256), BF16),
            pltpu.VMEM((rows, 256 * zs), BF16),
            pltpu.VMEM((rows, 8), F32),
            dma((5,)),
            dma((side, side)), dma((side, side)),
            dma((side, side)), dma((side, side)),
            dma((side, 2)), dma((side, 2)),
            dma((side, 2, 2, ring_slots)), dma((side, 2, 2, ring_slots)),
            dma((side, side)), dma((side, side)),
            dma((ep_size,)), dma((ep_size,)),
            dma((2, ring_slots)), dma((2, ring_slots)),
            dma((zs,)), dma((zs,)),
        ],
        compiler_params=pltpu.CompilerParams(
            collective_id=0, has_side_effects=True, vmem_limit_bytes=60 * 1024 * 1024
        ),
        name="whole",
    )(
        second_micro_input,
        expert_norm_gain[None, :],
        token_group_index,
        token_expert_pair.T,
        group_router_scores.T,
        expert_router_scores.T,
        expert_gate_weight,
        expert_up_weight,
        expert_down_weight,
        queries,
        values,
        forget_gate_logits,
        output_gate_logits,
        forget_gate_headroom,
        spike_log_decay,
        head_norm_gain[None, :],
        output_projection,
    )
    return tuple(result.astype(BF16) for result in results)


def solution(mesh):
    split = Mesh(mesh.devices.reshape(mesh.shape["ep"], 8, 2), ("ep", "tp_0", "tp_1"))
    placed = (
        P("ep", TP),
        P("ep", TP),
        P(None, "ep", TP),
        P("ep", TP),
        P(None, TP),
        P("ep"),
        P(TP),
        P(None, TP),
        P("ep", None),
        P(),
        P("ep"),
        P("ep", None),
        P("ep", None),
        P("ep", None),
        P("ep", None, TP),
        P("ep", None, TP),
        P("ep", TP, None),
    )
    return jax.shard_map(
        on_device,
        mesh=split,
        in_specs=placed,
        out_specs=(P("ep", TP), P("ep", TP)),
        check_vma=False,
    )
```
